256 devices in a mesh: sp: 64 (over z, y, core), tp: 4 (over x).
Axes of the slice: x: 4, y: 4, z: 8, core: 2. Of those that a mesh axis runs over, the one named last changes fastest.
Arguments:
- cotangent: bfloat16 [16384, 2048], P('sp'), may hold values from -16 to 16
- stream_in: bfloat16 [16384, 2048], P('sp'), may hold values from -6 to 6
- norm_gain: float32 [2048], replicated, may hold values from 0.1 to 1.9
- out_gate: bfloat16 [16384, 1024], P('sp', 'tp'), may hold values from -6 to 6
- in_gate: bfloat16 [16384, 1024], P('sp', 'tp'), may hold values from -6 to 6
- conv_input: bfloat16 [16384, 1024], P('sp', 'tp'), may hold values from -6 to 6
- conv_taps: float32 [3, 1024], P(None, 'tp'), may hold values from -3 to 3
- out_weight: bfloat16 [2048, 1024], P(None, 'tp'), may hold values from -0.1875 to 0.1875
- expert_gate: bfloat16 [64, 2048, 1024], P('sp', None, 'tp'), may hold values from -0.125 to 0.125
- expert_up: bfloat16 [64, 2048, 1024], P('sp', None, 'tp'), may hold values from -0.125 to 0.125
- expert_down: bfloat16 [64, 1024, 2048], P('sp', 'tp'), may hold values from -0.1875 to 0.1875
- expert_choice: int32 [16384, 2], P('sp'), may hold values from 0 to 63, all different within a row; in each aligned block of 256 rows (0 to 255, 256 to 511, ...) at most 16 rows name the same one
- route_scale: float32 [16384, 2], P('sp'), may hold values from 0.05 to 0.6
Outputs:
- grad_stream: bfloat16 [16384, 2048], P('sp', 'tp')
- grad_out_gate: bfloat16 [16384, 1024], P('sp', 'tp')
- grad_in_gate: bfloat16 [16384, 1024], P('sp', 'tp')
- grad_conv_input: bfloat16 [16384, 1024], P('sp', 'tp')
- grad_out_weight: float32 [2048, 1024], P('sp', 'tp')
- grad_expert_gate: float32 [64, 2048, 1024], P('sp', None, 'tp')
- grad_expert_up: float32 [64, 2048, 1024], P('sp', None, 'tp')
- grad_expert_down: float32 [64, 1024, 2048], P('sp', 'tp')
The draws below stay inside these ranges and needn't reach their ends.
Inputs may be any that keep to these rules, and one draw needn't show every extreme that they name: `expert_choice`: each row names two different experts. Within the rows of one device no expert is named more than 16 times, a bound that some block reaches in some devices' rows.
All inputs are finite; a program needn't handle non-finite values.
Results may differ from the reference program's by a relative error of at most 0.01.
Values may be sent and summed in bfloat16 or wider, within the bound.
No kernel may reach another device: no remote copies, remote signals or barrier semaphores. Data moves between devices by JAX's collectives and lax.ppermute only.
A program may use at most 128 MiB of HBM per device.

```python
import math
import jax
import jax.numpy as jnp
import numpy as np
from jax import lax

D = 2048
CW = 1024
FF = 1024
TAPS = 3
TOK_DEV = 256
TOKENS = 16384
EXPERTS = 64
CAP = 16
N_SP = 64
N_TP = 4


def raised(drawn, rng, source, target, shards_of, factor):
    def block_of(dim):
        return (jnp.arange(drawn.shape[dim]) // (drawn.shape[dim] // shards_of)).reshape((-1,) + (1,) * (drawn.ndim - 1 - dim))

    first = jax.random.permutation(rng, shards_of)[block_of(target)]
    other_side = (block_of(target) + shards_of // 2) % shards_of
    return jnp.where((block_of(source) == first) | (block_of(source) == other_side), factor * drawn, drawn)


def shard_levels(rng, dims, cuts, low, top_value):
    def one(axis_at, blocks):
        heights = jax.random.uniform(jax.random.fold_in(jax.random.fold_in(rng, 6), axis_at), (blocks,), jnp.float32, low / len(cuts), top_value / len(cuts))
        return jnp.repeat(jnp.exp(heights), dims[axis_at] // blocks).reshape((-1,) + (1,) * (len(dims) - axis_at - 1))

    factor_of = one(*cuts[0])
    for cut in cuts[1:]:
        factor_of = factor_of * one(*cut)
    return factor_of


def deal_out(key, own, number, rows, count, top, reach, slope):
    sequence = jax.random.permutation(key, count)
    heavy_load, common = load_shares(count, rows * top, reach, slope, True), load_shares(count, rows * top, reach, slope, False)
    places = jnp.arange(count)

    def named(lengths, offset_by):
        used = int((lengths > 0).sum())
        fixed = max(1, used // 4)
        passed = fixed + (places - fixed + offset_by * (used - fixed)) % max(1, count - fixed)
        return jnp.zeros((count,), jnp.int32).at[sequence[jnp.where(places < fixed, places, passed)]].set(jnp.asarray(lengths, jnp.int32))

    lengths = jnp.where(number % 4 == 0, named(heavy_load, number // 4), named(common, number - number // 4 - 1))
    mixed = jax.random.permutation(jax.random.fold_in(own, 3), count)
    source_of, sink = mixed[0:count // 2 * 2:2], mixed[1:count // 2 * 2:2]
    slack = jnp.minimum(lengths[source_of] - 1, reach - lengths[sink]) // 2
    slack = jnp.where((source_of == sequence[0]) | (sink == sequence[0]) | (lengths[sink] == 0), 0, jnp.maximum(slack, 0))
    passed = jax.random.randint(jax.random.fold_in(own, 4), (count // 2,), 0, 1 << 20) % (slack + 1)
    lengths = lengths.at[source_of].add(-passed).at[sink].add(passed)
    members = jnp.searchsorted(jnp.cumsum(lengths), jnp.arange(rows * top), side="right").astype(jnp.int32)
    grid = members.reshape(top, rows).T
    grid = grid[jax.random.permutation(jax.random.fold_in(own, 1), rows)]
    offset_by = jax.random.randint(jax.random.fold_in(own, 2), (rows, 1), 0, top)
    return jnp.take_along_axis(grid, (jnp.arange(top)[None, :] + offset_by) % top, axis=1)


def load_shares(number_of, total, most, slope, full):
    loads = [(1 << 20) // math.isqrt(standing ** slope) + 1 for standing in range(1, number_of + 1)]
    largest = most if full else min(most, max(-(-total // number_of), total * loads[0] // sum(loads)))
    least = 1 if total - largest >= number_of - 1 else 0
    holding, surplus = [largest] + [least] * (number_of - 1), total - largest - least * (number_of - 1)
    while surplus > 0:
        free = [i for i in range(1, number_of) if holding[i] < largest] or [i for i in range(1, number_of) if holding[i] < most]
        pool, left = sum([loads[i] for i in free]), surplus
        for i in free:
            more = min(most - holding[i], max(1, left * loads[i] // pool), surplus)
            holding[i] = holding[i] + more
            surplus = surplus - more
    return np.array(holding)


def normal_values(rng, shape, spread, reach, cuts=(), kind=jnp.bfloat16):
    array = spread * jax.random.normal(rng, shape, jnp.float32)
    if cuts:
        array = array * shard_levels(rng, shape, cuts, -0.22, 0.18)
    return jnp.clip(array, -reach, reach).astype(kind)


def gaussian_with(own_key, extent, width, most, pieces, heavy, kind=jnp.bfloat16):
    values = width * jax.random.normal(own_key, extent, jnp.float32)
    if pieces:
        values = values * shard_levels(own_key, extent, pieces, -0.22, 0.18)
    return jnp.clip(raised(values, jax.random.fold_in(own_key, 3), *heavy), -most, most).astype(kind)


def setup_inputs(seed: int = 0) -> dict:
    streams_of = jax.random.split(jax.random.key(seed), 14)
    cotangent = gaussian_with(streams_of[0], (TOKENS, D), 1.0, 16.0, ((0, 64),), (0, 1, 64, 4.0))
    stream_in = normal_values(streams_of[1], (TOKENS, D), 1.0, 6.0, ((0, 64),))
    norm_gain = jnp.clip(1.0 + 0.18 * jax.random.normal(streams_of[2], (D,), jnp.float32), 0.1, 1.9)
    out_gate = normal_values(streams_of[3], (TOKENS, CW), 1.0, 6.0, ((0, 64), (1, 4)))
    in_gate = normal_values(streams_of[4], (TOKENS, CW), 1.0, 6.0, ((0, 64), (1, 4)))
    conv_input = normal_values(streams_of[5], (TOKENS, CW), 1.0, 6.0, ((0, 64), (1, 4)))
    conv_taps = normal_values(streams_of[6], (TAPS, CW), 0.577, 3.0, ((1, 4),), jnp.float32)
    out_weight = normal_values(streams_of[7], (D, CW), CW ** -0.5, 0.1875, ((1, 4),))
    expert_gate = normal_values(streams_of[8], (EXPERTS, D, FF), D ** -0.5, 0.125, ((0, 64), (2, 4)))
    expert_up = normal_values(streams_of[9], (EXPERTS, D, FF), D ** -0.5, 0.125, ((0, 64), (2, 4)))
    expert_down = normal_values(streams_of[10], (EXPERTS, FF, D), FF ** -0.5, 0.1875, ((0, 64), (1, 4)))
    expert_choice_keys = jax.random.split(jax.random.fold_in(streams_of[11], 1), TOKENS // TOK_DEV)
    expert_choice_turns = jax.random.permutation(jax.random.fold_in(streams_of[11], 3), TOKENS // TOK_DEV)
    expert_choice = jax.vmap(lambda own, number: deal_out(jax.random.fold_in(streams_of[11], 2), own, number, TOK_DEV, EXPERTS, 2, CAP, 2))(expert_choice_keys, expert_choice_turns).reshape((TOKENS, 2))
    route_scale = jnp.clip(0.05 + 0.55 * jax.random.uniform(streams_of[12], (TOKENS, 2), jnp.float32) ** shard_levels(streams_of[12], (TOKENS, 2), ((0, 64),), -0.2, 0.2), 0.05, 0.6)
    return {"cotangent": cotangent, "stream_in": stream_in, "norm_gain": norm_gain, "out_gate": out_gate, "in_gate": in_gate, "conv_input": conv_input, "conv_taps": conv_taps, "out_weight": out_weight, "expert_gate": expert_gate, "expert_up": expert_up, "expert_down": expert_down, "expert_choice": expert_choice, "route_scale": route_scale}


norm_eps = 1e-06

def slot_table(choice_rows, expert_count, capacity):
    flat_ids = choice_rows.reshape(-1).astype(jnp.int32)
    route_count = flat_ids.shape[0]
    onehot = (flat_ids[:, None] == jnp.arange(expert_count, dtype=jnp.int32)[None, :]).astype(jnp.int32)
    earlier = jnp.cumsum(onehot, axis=0) - onehot
    position = lax.optimization_barrier(jnp.sum(earlier * onehot, axis=1)).astype(jnp.int32)
    slot_of_route = (flat_ids * capacity + position).astype(jnp.int32)
    route_of_slot = jnp.full((expert_count * capacity,), route_count, jnp.int32)
    route_of_slot = route_of_slot.at[slot_of_route].set(jnp.arange(route_count, dtype=jnp.int32))
    return (slot_of_route, route_of_slot)

def rows_product(left, right):
    return lax.dot_general(left, right, (((0,), (0,)), ((), ())), preferred_element_type=jnp.float32)

def cols_product(left, right):
    return lax.dot_general(left, right, (((1,), (1,)), ((), ())), preferred_element_type=jnp.float32)

def reference(cotangent, stream_in, norm_gain, out_gate, in_gate, conv_input, conv_taps, out_weight, expert_gate, expert_up, expert_down, expert_choice, route_scale):
    stream = stream_in.astype(jnp.float32)
    inverse_rms = lax.rsqrt(lax.optimization_barrier(jnp.mean(stream * stream, axis=-1, keepdims=True)) + norm_eps)
    unit_stream = stream * inverse_rms
    normed = (unit_stream * norm_gain.astype(jnp.float32)).astype(jnp.bfloat16)
    capacity = 4 * TOK_DEV // N_SP
    route_count = 2 * TOK_DEV
    block_ids = expert_choice.reshape(N_SP, TOK_DEV, 2)
    tables = jax.vmap(lambda choice_block: slot_table(choice_block, EXPERTS, capacity)[1])(block_ids)
    flat_scale = route_scale.reshape(-1)
    source_base = (jnp.arange(N_SP, dtype=jnp.int32) * route_count)[:, None]
    width_tp = FF // N_TP

    def expert_step(accum, inputs):
        w_gate, w_up, w_down, expert = inputs
        chosen = lax.dynamic_slice_in_dim(tables, (expert * capacity).astype(jnp.int32), capacity, 1)
        present = chosen < route_count
        routes = (source_base + jnp.where(present, chosen, 0)).reshape(-1).astype(jnp.int32)
        present = present.reshape(-1)
        token = (routes // 2).astype(jnp.int32)
        weight = jnp.where(present, flat_scale[routes], jnp.zeros((), jnp.float32))
        scaled_cot = (cotangent[token].astype(jnp.float32) * weight[:, None]).astype(jnp.bfloat16)
        expert_rows = jnp.where(present[:, None], normed[token], jnp.zeros((), jnp.bfloat16))
        gate_pre = jnp.dot(expert_rows, w_gate, preferred_element_type=jnp.float32)
        up_pre = jnp.dot(expert_rows, w_up, preferred_element_type=jnp.float32)
        sigmoid_gate = jax.nn.sigmoid(gate_pre)
        silu_gate = gate_pre * sigmoid_gate
        hidden = (silu_gate * up_pre).astype(jnp.bfloat16)
        grad_down = rows_product(hidden, scaled_cot)
        hidden_grad = cols_product(scaled_cot, w_down)
        gate_grad = (hidden_grad * up_pre * sigmoid_gate * (1.0 + gate_pre * (1.0 - sigmoid_gate))).astype(jnp.bfloat16)
        up_grad = (hidden_grad * silu_gate).astype(jnp.bfloat16)
        grad_gate = rows_product(expert_rows, gate_grad)
        grad_up = rows_product(expert_rows, up_grad)
        slot_rows = expert_rows.shape[0]
        shares = jnp.einsum('rpf,dpf->prd', gate_grad.astype(jnp.float32).reshape(slot_rows, N_TP, width_tp), w_gate.astype(jnp.float32).reshape(D, N_TP, width_tp))
        shares = shares + jnp.einsum('rpf,dpf->prd', up_grad.astype(jnp.float32).reshape(slot_rows, N_TP, width_tp), w_up.astype(jnp.float32).reshape(D, N_TP, width_tp))
        rounded = lax.optimization_barrier(shares.astype(jnp.bfloat16))
        slot_grad = lax.optimization_barrier(jnp.sum(rounded.astype(jnp.float32), axis=0)).astype(jnp.bfloat16)
        slot_grad = lax.optimization_barrier(slot_grad)
        accum = accum.at[token].add(jnp.where(present[:, None], slot_grad.astype(jnp.float32), jnp.zeros((), jnp.float32)))
        return (accum, (grad_gate, grad_up, grad_down))
    start_accum = jnp.zeros((TOKENS, D), jnp.float32)
    accum, grads = lax.scan(expert_step, start_accum, (expert_gate, expert_up, expert_down, jnp.arange(EXPERTS, dtype=jnp.int32)))
    grad_gate, grad_up, grad_down = grads
    token_grad = lax.optimization_barrier(accum.astype(jnp.bfloat16))
    unit_grad = token_grad.astype(jnp.float32) * norm_gain.astype(jnp.float32)
    along = lax.optimization_barrier(jnp.mean(unit_stream * unit_grad, axis=-1, keepdims=True))
    stream_grad = (cotangent.astype(jnp.float32) + inverse_rms * (unit_grad - unit_stream * along)).astype(jnp.bfloat16)
    taps = conv_taps.astype(jnp.float32)
    product = in_gate.astype(jnp.float32) * conv_input.astype(jnp.float32)
    padded = jnp.pad(product, ((2, 0), (0, 0)))
    filtered = taps[0] * product + taps[1] * padded[1:-1] + taps[2] * padded[:-2]
    mixed_in = (out_gate.astype(jnp.float32) * filtered).astype(jnp.bfloat16)
    mixed_grad = jnp.dot(stream_grad, out_weight, preferred_element_type=jnp.float32)
    grad_out_gate = (mixed_grad * filtered).astype(jnp.bfloat16)
    filtered_grad = mixed_grad * out_gate.astype(jnp.float32)
    padded_grad = jnp.pad(filtered_grad, ((0, 2), (0, 0)))
    product_grad = taps[0] * filtered_grad + taps[1] * padded_grad[1:-1] + taps[2] * padded_grad[2:]
    grad_in_gate = (product_grad * conv_input.astype(jnp.float32)).astype(jnp.bfloat16)
    grad_conv_input = (product_grad * in_gate.astype(jnp.float32)).astype(jnp.bfloat16)
    grad_out_weight = rows_product(stream_grad, mixed_in)
    return (stream_grad, grad_out_gate, grad_in_gate, grad_conv_input, grad_out_weight, grad_gate, grad_up, grad_down)
```

```python
import jax
import jax.numpy as jnp
from jax import lax
from jax.experimental import pallas as pl
from jax.experimental.pallas import tpu as pltpu
from jax.sharding import PartitionSpec as P

norm_eps = 1e-06
bf16 = jnp.bfloat16
f32 = jnp.float32


WHOLE = pl.BlockSpec(memory_space=pltpu.VMEM)
SCALAR = pl.BlockSpec(memory_space=pltpu.SMEM)


def call(body, outs, operands, name, flops=0, moved=0, limit=60 * 1024 * 1024):
    return pl.pallas_call(
        body,
        out_shape=[jax.ShapeDtypeStruct(shape, dtype) for shape, dtype in outs],
        in_specs=[SCALAR] + [WHOLE] * (len(operands) - 1),
        out_specs=[WHOLE] * len(outs),
        name=name,
        cost_estimate=pl.CostEstimate(flops=flops, bytes_accessed=moved, transcendentals=0),
        compiler_params=pltpu.CompilerParams(vmem_limit_bytes=limit),
    )(*operands)


def dot(left, right, contract):
    return lax.dot_general(
        left, right, ((contract[:1], contract[1:]), ((), ())), preferred_element_type=f32
    )


def ring(size, steps):
    return [(k, (k + steps) % size) for k in range(size)]


def unit_rows(stream_ref):
    stream = stream_ref[...].astype(f32)
    inverse_rms = lax.rsqrt(jnp.mean(stream * stream, axis=-1, keepdims=True) + norm_eps)
    return stream * inverse_rms, inverse_rms


def send_kernel(tp_ref, choice_ref, scale_ref, stream_ref, gain_ref, cot_ref, send_ref, pick_ref):
    tokens, width = stream_ref.shape
    experts, double, columns = send_ref.shape
    capacity = double // 2
    start = pl.multiple_of(tp_ref[0] * columns, columns)
    choice = choice_ref[...]
    expert_iota = lax.broadcasted_iota(jnp.int32, (tokens, experts), 1)
    first = choice[:, 0:1] == expert_iota
    second = choice[:, 1:2] == expert_iota
    named = jnp.where(first | second, 1.0, 0.0).astype(bf16)
    row = lax.broadcasted_iota(jnp.int32, (tokens, tokens), 0)
    col = lax.broadcasted_iota(jnp.int32, (tokens, tokens), 1)
    before = jnp.where(col < row, 1.0, 0.0).astype(bf16)
    earlier = dot(before, named, (1, 0))
    place_first = jnp.sum(jnp.where(first, earlier, 0.0), axis=1, keepdims=True).astype(jnp.int32)
    place_second = jnp.sum(jnp.where(second, earlier, 0.0), axis=1, keepdims=True).astype(jnp.int32)
    slot_iota = lax.broadcasted_iota(jnp.int32, (tokens, experts * capacity), 1)
    pick_first = choice[:, 0:1] * capacity + place_first == slot_iota
    pick_second = choice[:, 1:2] * capacity + place_second == slot_iota
    pick_both = jnp.where(pick_first | pick_second, 1.0, 0.0).astype(bf16)
    pick_ref[...] = pick_both
    unit, _ = unit_rows(stream_ref)
    stream_cols = stream_ref[:, pl.ds(start, columns)].astype(f32)
    _, inverse_rms = unit_rows(stream_ref)
    normed = (stream_cols * inverse_rms * gain_ref[:, pl.ds(start, columns)]).astype(bf16)
    rows = dot(pick_both, normed, (0, 0)).astype(bf16)
    send_ref[:, :capacity, :] = rows.reshape(experts, capacity, columns)
    cot = cot_ref[:, pl.ds(start, columns)].astype(f32)
    scale = scale_ref[...]
    scaled_first = (cot * scale[:, 0:1]).astype(bf16)
    scaled_second = (cot * scale[:, 1:2]).astype(bf16)
    scaled = dot(jnp.where(pick_first, 1.0, 0.0).astype(bf16), scaled_first, (0, 0)) + dot(
        jnp.where(pick_second, 1.0, 0.0).astype(bf16), scaled_second, (0, 0)
    )
    send_ref[:, capacity:, :] = scaled.astype(bf16).reshape(experts, capacity, columns)


def expert_kernel(
    tp_ref, r0, r1, r2, r3, s0, s1, s2, s3, gate_ref, up_ref, down_ref,
    hidden_ref, ggrad_ref, ugrad_ref, p0, p1a, p1b, p2a, p2b, p3a, p3b,
):
    columns = r0.shape[1]
    half = r0.shape[0] // 2
    start = [
        pl.multiple_of(lax.rem(tp_ref[0] + j, 4) * columns, columns) for j in range(4)
    ]
    rows = (r0, r1, r2, r3)
    scaled = (s0, s1, s2, s3)
    gate_pre = sum(dot(rows[j][...], gate_ref[0, pl.ds(start[j], columns), :], (1, 0)) for j in range(4))
    up_pre = sum(dot(rows[j][...], up_ref[0, pl.ds(start[j], columns), :], (1, 0)) for j in range(4))
    hidden_grad = sum(
        dot(scaled[j][...], down_ref[0, :, pl.ds(start[j], columns)], (1, 1)) for j in range(4)
    )
    sigmoid_gate = jax.nn.sigmoid(gate_pre)
    silu_gate = gate_pre * sigmoid_gate
    hidden_ref[...] = (silu_gate * up_pre).astype(bf16)
    gate_grad = (
        hidden_grad * up_pre * sigmoid_gate * (1.0 + gate_pre * (1.0 - sigmoid_gate))
    ).astype(bf16)
    up_grad = (hidden_grad * silu_gate).astype(bf16)
    ggrad_ref[...] = gate_grad
    ugrad_ref[...] = up_grad
    outs = ((p0,), (p1a, p1b), (p2a, p2b), (p3a, p3b))
    for j in (2, 1, 3, 0):
        partial = (
            dot(gate_grad, gate_ref[0, pl.ds(start[j], columns), :], (1, 1))
            + dot(up_grad, up_ref[0, pl.ds(start[j], columns), :], (1, 1))
        ).astype(bf16)
        if j == 0:
            p0[...] = partial
        else:
            outs[j][0][...] = partial[:half]
            outs[j][1][...] = partial[half:]


def weights_kernel(tp_ref, *refs):
    chunks = (len(refs) - 3) // 11
    outs = refs[-3:]
    columns = refs[0].shape[1]
    for j in range(4):
        start = pl.multiple_of(lax.rem(tp_ref[0] + j, 4) * columns, columns)
        gate = up = down = 0.0
        for c in range(chunks):
            part = refs[11 * c : 11 * c + 11]
            rows, scaled = part[j][...], part[4 + j][...]
            hidden, gate_grad, up_grad = (part[8 + k][...] for k in range(3))
            gate = gate + dot(rows, gate_grad, (0, 0))
            up = up + dot(rows, up_grad, (0, 0))
            down = down + dot(hidden, scaled, (0, 0))
        outs[0][0, pl.ds(start, columns), :] = gate
        outs[1][0, pl.ds(start, columns), :] = up
        outs[2][0, :, pl.ds(start, columns)] = down


def tail_kernel(
    tp_ref, t0, t1, t2a, t2b, t3, stream_ref, cot_ref, gain_ref, weight_ref, filtered_ref, gate_ref,
    mixed_in_ref, gstream_ref, ggate_ref, fgrad_ref, wgrad_ref,
):
    tokens, columns = t0.shape
    unit, inverse_rms = unit_rows(stream_ref)
    starts = [pl.multiple_of(lax.rem(tp_ref[0] + j, 4) * columns, columns) for j in range(4)]
    opposite = jnp.concatenate([t2a[...], t2b[...]], axis=0)
    pieces = (t0[...], t1[...], opposite, t3[...])
    unit_cols, unit_grads = [], []
    along = 0.0
    for j in range(4):
        unit_col = stream_ref[:, pl.ds(starts[j], columns)].astype(f32) * inverse_rms
        unit_grad = pieces[j].astype(f32) * gain_ref[:, pl.ds(starts[j], columns)]
        along = along + jnp.sum(unit_col * unit_grad, axis=-1, keepdims=True)
        unit_cols.append(unit_col)
        unit_grads.append(unit_grad)
    along = along * (1.0 / (4 * columns))
    mixed_grad = 0.0
    grads = []
    for j in range(4):
        grad = (
            cot_ref[:, pl.ds(starts[j], columns)].astype(f32)
            + inverse_rms * (unit_grads[j] - unit_cols[j] * along)
        ).astype(bf16)
        if j == 0:
            gstream_ref[...] = grad
        grads.append(grad)
        mixed_grad = mixed_grad + dot(grad, weight_ref[pl.ds(starts[j], columns), :], (1, 0))
    ggate_ref[...] = (mixed_grad * filtered_ref[...]).astype(bf16)
    fgrad_ref[...] = mixed_grad * gate_ref[...].astype(f32)
    mixed_in = mixed_in_ref[...]
    for j in range(4):
        wgrad_ref[pl.ds(starts[j], columns), :] = dot(grads[j], mixed_in, (0, 0)).astype(bf16)


def shift_edge(value, axis, steps):
    count = lax.axis_size(axis)
    first, last = (max(0, -steps), min(count, count - steps))
    return lax.ppermute(value, axis, [(source, source + steps) for source in range(first, last)])


def exchange(array, axis, groups=None):
    return lax.all_to_all(
        array, axis, split_axis=0, concat_axis=0, tiled=True, axis_index_groups=groups
    )


def shards(
    cotangent, stream_in, norm_gain, out_gate, in_gate, conv_input, conv_taps, out_weight,
    expert_gate, expert_up, expert_down, expert_choice, route_scale,
):
    sp_size = lax.axis_size("sp")
    tp_size = lax.axis_size("tp")
    tokens, width = stream_in.shape
    columns = width // tp_size
    capacity = 4 * tokens // sp_size
    chunks = 2
    part = capacity // chunks
    right, left = ring(tp_size, 1), ring(tp_size, -1)
    tp = lax.axis_index("tp").astype(jnp.int32).reshape(1)
    gain = norm_gain.reshape(1, width)

    send, pick = call(
        send_kernel,
        [((sp_size, 2 * capacity, columns), bf16), ((tokens, sp_size * capacity), bf16)],
        [tp, expert_choice, route_scale, stream_in, gain, cotangent],
        "pick_slots",
    )
    arrived = exchange(send, "sp")

    gathered = []
    for c in range(chunks):
        here = [
            arrived[:, k * capacity + c * part : k * capacity + (c + 1) * part]
            .reshape(sp_size * part, columns)
            for k in range(2)
        ]
        before = [lax.ppermute(h, "tp", right) for h in here]
        after = [lax.ppermute(h, "tp", left) for h in here]
        opposite = [lax.ppermute(before[0], "tp", right), lax.ppermute(after[1], "tp", left)]
        gathered.append(
            [blocks[k] for k in range(2) for blocks in (here, after, opposite, before)]
        )

    returned = []
    saved = []
    rows_here = sp_size * part
    ff = expert_gate.shape[2]
    half = rows_here // 2
    for c in range(chunks):
        outs = call(
            expert_kernel,
            [((rows_here, ff), bf16)] * 3
            + [((rows_here, columns), bf16)]
            + [((half, columns), bf16)] * 6,
            [tp, *gathered[c], expert_gate, expert_up, expert_down],
            f"expert_chunk",
            flops=10 * rows_here * width * ff,
        )
        saved += [*gathered[c], *outs[:3]]
        p0, p1a, p1b, p2a, p2b, p3a, p3b = outs[3:]
        to_next = lax.ppermute(p2a, "tp", right)
        to_last = lax.ppermute(p2b, "tp", left)
        from_last_b = lax.ppermute(p1b, "tp", right)
        from_next_a = lax.ppermute(p3a, "tp", left)
        p1a = (p1a.astype(f32) + to_next.astype(f32)).astype(bf16)
        p3b = (p3b.astype(f32) + to_last.astype(f32)).astype(bf16)
        from_last_a = lax.ppermute(p1a, "tp", right)
        from_next_b = lax.ppermute(p3b, "tp", left)
        slot_grad = (
            p0.reshape(2, half, columns).astype(f32)
            + jnp.stack([from_last_a, from_last_b]).astype(f32)
            + jnp.stack([from_next_a, from_next_b]).astype(f32)
        ).astype(bf16)
        returned.append(exchange(slot_grad.reshape(sp_size, part, columns), "sp"))

    grad_gate, grad_up, grad_down = call(
        weights_kernel,
        [(expert_gate.shape, f32), (expert_up.shape, f32), (expert_down.shape, f32)],
        [tp, *saved],
        "expert_weights",
        flops=6 * sp_size * capacity * width * ff,
    )

    product = in_gate.astype(f32) * conv_input.astype(f32)
    earlier = shift_edge(product[-2:], "sp", 1)
    extended = jnp.concatenate([earlier, product], axis=0)
    filtered = conv_taps[0] * product + conv_taps[1] * extended[1:-1] + conv_taps[2] * extended[:-2]
    mixed_in = (out_gate.astype(f32) * filtered).astype(bf16)

    pick = pick.reshape(tokens, sp_size, chunks, part)
    token_cols = sum(
        jnp.dot(
            pick[:, :, c].reshape(tokens, sp_size * part),
            returned[c].reshape(sp_size * part, columns),
            preferred_element_type=f32,
        )
        for c in range(chunks)
    ).astype(bf16)
    t3 = lax.ppermute(token_cols, "tp", right)
    t1 = lax.ppermute(token_cols, "tp", left)
    t2a = lax.ppermute(t3[: tokens // 2], "tp", right)
    t2b = lax.ppermute(t1[tokens // 2 :], "tp", left)
    grad_stream, grad_out_gate, filtered_grad, weight_grad = call(
        tail_kernel,
        [
            ((tokens, columns), bf16),
            (out_gate.shape, bf16),
            (out_gate.shape, f32),
            (out_weight.shape, bf16),
        ],
        [tp, token_cols, t1, t2a, t2b, t3, stream_in, cotangent, gain, out_weight, filtered, out_gate, mixed_in],
        "stream_tail",
    )
    later = shift_edge(filtered_grad[:2], "sp", -1)
    extended_grad = jnp.concatenate([filtered_grad, later], axis=0)
    product_grad = (
        conv_taps[0] * filtered_grad
        + conv_taps[1] * extended_grad[1:-1]
        + conv_taps[2] * extended_grad[2:]
    )
    grad_in_gate = (product_grad * conv_input.astype(f32)).astype(bf16)
    grad_conv_input = (product_grad * in_gate.astype(f32)).astype(bf16)

    core = lax.rem(lax.axis_index("sp"), 2)
    pairs = weight_grad.reshape(sp_size // 2, 2, width // sp_size, out_weight.shape[1])
    keep = lax.dynamic_index_in_dim(pairs, core, 1, keepdims=False)
    give = lax.dynamic_index_in_dim(pairs, 1 - core, 1, keepdims=False)
    taken = lax.ppermute(give, "sp", [(k, k ^ 1) for k in range(sp_size)])
    keep = (keep.astype(f32) + taken.astype(f32)).astype(bf16)
    same_core = [[2 * k + c for k in range(sp_size // 2)] for c in range(2)]
    grad_out_weight = exchange(keep, "sp", same_core).astype(f32).sum(axis=0)
    return (
        grad_stream, grad_out_gate, grad_in_gate, grad_conv_input, grad_out_weight,
        grad_gate, grad_up, grad_down,
    )


def solution(mesh):
    return jax.shard_map(
        shards,
        mesh=mesh,
        in_specs=(
            P("sp", None), P("sp", None), P(), P("sp", "tp"), P("sp", "tp"), P("sp", "tp"),
            P(None, "tp"), P(None, "tp"), P("sp", None, "tp"), P("sp", None, "tp"),
            P("sp", "tp", None), P("sp", None), P("sp", None),
        ),
        out_specs=(
            P("sp", "tp"), P("sp", "tp"), P("sp", "tp"), P("sp", "tp"), P("sp", "tp"),
            P("sp", None, "tp"), P("sp", None, "tp"), P("sp", "tp", None),
        ),
        check_vma=False,
    )
```

```python
import jax
import jax.numpy as jnp
from jax import lax
from jax.experimental import pallas as pl
from jax.experimental.pallas import tpu as pltpu
from jax.sharding import PartitionSpec as P

norm_eps = 1e-06
bf16 = jnp.bfloat16
f32 = jnp.float32


WHOLE = pl.BlockSpec(memory_space=pltpu.VMEM)
SCALAR = pl.BlockSpec(memory_space=pltpu.SMEM)


def call(body, outs, operands, name, flops=0, moved=0, limit=60 * 1024 * 1024):
    return pl.pallas_call(
        body,
        out_shape=[jax.ShapeDtypeStruct(shape, dtype) for shape, dtype in outs],
        in_specs=[SCALAR] + [WHOLE] * (len(operands) - 1),
        out_specs=[WHOLE] * len(outs),
        name=name,
        cost_estimate=pl.CostEstimate(flops=flops, bytes_accessed=moved, transcendentals=0),
        compiler_params=pltpu.CompilerParams(vmem_limit_bytes=limit),
    )(*operands)


def dot(left, right, contract):
    return lax.dot_general(
        left, right, ((contract[:1], contract[1:]), ((), ())), preferred_element_type=f32
    )


def ring(size, steps):
    return [(k, (k + steps) % size) for k in range(size)]


def unit_rows(stream_ref):
    stream = stream_ref[...].astype(f32)
    inverse_rms = lax.rsqrt(jnp.mean(stream * stream, axis=-1, keepdims=True) + norm_eps)
    return stream * inverse_rms, inverse_rms


def send_kernel(tp_ref, choice_ref, scale_ref, stream_ref, gain_ref, cot_ref, *outs):
    tokens, width = stream_ref.shape
    chunks = len(outs) // 2
    experts, part, columns = outs[0].shape
    part = part // 2
    start = pl.multiple_of(tp_ref[0] * columns, columns)
    first_id, second_id = choice_ref[0:1, :], choice_ref[1:2, :]
    expert_iota = lax.broadcasted_iota(jnp.int32, (experts, tokens), 0)
    first, second = first_id == expert_iota, second_id == expert_iota
    named = jnp.where(first | second, 1.0, 0.0).astype(bf16)
    row = lax.broadcasted_iota(jnp.int32, (tokens, tokens), 0)
    col = lax.broadcasted_iota(jnp.int32, (tokens, tokens), 1)
    before = jnp.where(row < col, 1.0, 0.0).astype(bf16)
    earlier = dot(named, before, (1, 0))
    slots = []
    for chosen, ids in ((first, first_id), (second, second_id)):
        place = jnp.sum(jnp.where(chosen, earlier, 0.0), axis=0, keepdims=True).astype(jnp.int32)
        chunk = lax.div(place, part)
        slots.append(chunk * (experts * part) + ids * part + (place - chunk * part))
    _, inverse_rms = unit_rows(stream_ref)
    stream_cols = stream_ref[:, pl.ds(start, columns)].astype(f32)
    normed = (stream_cols * inverse_rms * gain_ref[:, pl.ds(start, columns)]).astype(bf16)
    cot = cot_ref[:, pl.ds(start, columns)]
    slot_iota = lax.broadcasted_iota(jnp.int32, (experts * part, tokens), 0)
    for c in range(chunks):
        send_ref, pick_ref = outs[2 * c : 2 * c + 2]
        here = slot_iota + c * experts * part
        pick_first, pick_second = slots[0] == here, slots[1] == here
        pick = jnp.where(pick_first | pick_second, 1.0, 0.0).astype(bf16)
        pick_ref[...] = pick
        send_ref[:, :part, :] = dot(pick, normed, (1, 0)).astype(bf16).reshape(experts, part, columns)
        scale = jnp.where(pick_first, scale_ref[0:1, :], 0.0) + jnp.where(
            pick_second, scale_ref[1:2, :], 0.0
        )
        weight = jnp.sum(scale, axis=1, keepdims=True)
        send_ref[:, part:, :] = (
            (dot(pick, cot, (1, 0)) * weight).astype(bf16).reshape(experts, part, columns)
        )


def expert_kernel(
    tp_ref, r0, r1, r2, r3, s0, s1, s2, s3, gate_ref, up_ref, down_ref,
    hidden_ref, ggrad_ref, ugrad_ref, p0, p1, p2a, p2b, p3,
):
    columns = r0.shape[1]
    half = r0.shape[0] // 2
    start = [
        pl.multiple_of(lax.rem(tp_ref[0] + j, 4) * columns, columns) for j in range(4)
    ]
    rows = (r0, r1, r2, r3)
    scaled = (s0, s1, s2, s3)
    gate_pre = sum(dot(rows[j][...], gate_ref[0, pl.ds(start[j], columns), :], (1, 0)) for j in range(4))
    up_pre = sum(dot(rows[j][...], up_ref[0, pl.ds(start[j], columns), :], (1, 0)) for j in range(4))
    hidden_grad = sum(
        dot(scaled[j][...], down_ref[0, :, pl.ds(start[j], columns)], (1, 1)) for j in range(4)
    )
    sigmoid_gate = jax.nn.sigmoid(gate_pre)
    silu_gate = gate_pre * sigmoid_gate
    hidden_ref[...] = (silu_gate * up_pre).astype(bf16)
    gate_grad = (
        hidden_grad * up_pre * sigmoid_gate * (1.0 + gate_pre * (1.0 - sigmoid_gate))
    ).astype(bf16)
    up_grad = (hidden_grad * silu_gate).astype(bf16)
    ggrad_ref[...] = gate_grad
    ugrad_ref[...] = up_grad
    for j in (2, 1, 3, 0):
        partial = (
            dot(gate_grad, gate_ref[0, pl.ds(start[j], columns), :], (1, 1))
            + dot(up_grad, up_ref[0, pl.ds(start[j], columns), :], (1, 1))
        ).astype(bf16)
        if j == 2:
            p2a[...] = partial[:half]
            p2b[...] = partial[half:]
        else:
            (p0, p1, None, p3)[j][...] = partial


def weights_kernel(tp_ref, *refs):
    chunks = (len(refs) - 3) // 11
    outs = refs[-3:]
    columns = refs[0].shape[1]
    for j in range(4):
        start = pl.multiple_of(lax.rem(tp_ref[0] + j, 4) * columns, columns)
        gate = up = down = 0.0
        for c in range(chunks):
            part = refs[11 * c : 11 * c + 11]
            rows, scaled = part[j][...], part[4 + j][...]
            hidden, gate_grad, up_grad = (part[8 + k][...] for k in range(3))
            gate = gate + dot(rows, gate_grad, (0, 0))
            up = up + dot(rows, up_grad, (0, 0))
            down = down + dot(hidden, scaled, (0, 0))
        outs[0][0, pl.ds(start, columns), :] = gate
        outs[1][0, pl.ds(start, columns), :] = up
        outs[2][0, :, pl.ds(start, columns)] = down


def token_kernel(tp_ref, *refs):
    total = 0.0
    for c in range(len(refs) // 2):
        pick, back = refs[2 * c][...], refs[2 * c + 1][...]
        total = total + dot(pick, back.reshape(pick.shape[0], back.shape[2]), (0, 0))
    refs[-1][...] = total.astype(bf16)


def tail_kernel(
    tp_ref, t0, t1, t2a, t2b, t3, stream_ref, cot_ref, gain_ref, weight_ref, filtered_ref, gate_ref,
    mixed_in_ref, gstream_ref, ggate_ref, fgrad_ref, wgrad_ref,
):
    tokens, columns = t0.shape
    unit, inverse_rms = unit_rows(stream_ref)
    starts = [pl.multiple_of(lax.rem(tp_ref[0] + j, 4) * columns, columns) for j in range(4)]
    opposite = jnp.concatenate([t2a[...], t2b[...]], axis=0)
    pieces = (t0[...], t1[...], opposite, t3[...])
    unit_cols, unit_grads = [], []
    along = 0.0
    for j in range(4):
        unit_col = stream_ref[:, pl.ds(starts[j], columns)].astype(f32) * inverse_rms
        unit_grad = pieces[j].astype(f32) * gain_ref[:, pl.ds(starts[j], columns)]
        along = along + jnp.sum(unit_col * unit_grad, axis=-1, keepdims=True)
        unit_cols.append(unit_col)
        unit_grads.append(unit_grad)
    along = along * (1.0 / (4 * columns))
    mixed_grad = 0.0
    grads = []
    for j in range(4):
        grad = (
            cot_ref[:, pl.ds(starts[j], columns)].astype(f32)
            + inverse_rms * (unit_grads[j] - unit_cols[j] * along)
        ).astype(bf16)
        if j == 0:
            gstream_ref[...] = grad
        grads.append(grad)
        mixed_grad = mixed_grad + dot(grad, weight_ref[pl.ds(starts[j], columns), :], (1, 0))
    ggate_ref[...] = (mixed_grad * filtered_ref[...]).astype(bf16)
    fgrad_ref[...] = mixed_grad * gate_ref[...].astype(f32)
    mixed_in = mixed_in_ref[...]
    for j in range(4):
        wgrad_ref[pl.ds(starts[j], columns), :] = dot(grads[j], mixed_in, (0, 0)).astype(bf16)


def shift_edge(value, axis, steps):
    count = lax.axis_size(axis)
    first, last = (max(0, -steps), min(count, count - steps))
    return lax.ppermute(value, axis, [(source, source + steps) for source in range(first, last)])


def exchange(array, axis, groups=None):
    return lax.all_to_all(
        array, axis, split_axis=0, concat_axis=0, tiled=True, axis_index_groups=groups
    )


def shards(
    cotangent, stream_in, norm_gain, out_gate, in_gate, conv_input, conv_taps, out_weight,
    expert_gate, expert_up, expert_down, expert_choice, route_scale,
):
    sp_size = lax.axis_size("sp")
    tp_size = lax.axis_size("tp")
    tokens, width = stream_in.shape
    columns = width // tp_size
    capacity = 4 * tokens // sp_size
    chunks = 2
    part = capacity // chunks
    right, left = ring(tp_size, 1), ring(tp_size, -1)
    tp = lax.axis_index("tp").astype(jnp.int32).reshape(1)
    gain = norm_gain.reshape(1, width)

    block = ((sp_size, 2 * part, columns), bf16)
    sent = call(
        send_kernel,
        [block, ((sp_size * part, tokens), bf16)] * chunks,
        [tp, expert_choice.T, route_scale.T, stream_in, gain, cotangent],
        "pick_slots",
    )
    picks = sent[1::2]

    gathered = []
    for c in range(chunks):
        both = exchange(sent[2 * c], "sp")
        here = [
            both[:, k * part : (k + 1) * part].reshape(sp_size * part, columns) for k in range(2)
        ]
        before = [lax.ppermute(h, "tp", right) for h in here]
        after = [lax.ppermute(h, "tp", left) for h in here]
        opposite = [lax.ppermute(before[0], "tp", right), lax.ppermute(after[1], "tp", left)]
        gathered.append(
            [blocks[k] for k in range(2) for blocks in (here, after, opposite, before)]
        )

    returned = []
    saved = []
    rows_here = sp_size * part
    ff = expert_gate.shape[2]
    half = rows_here // 2
    for c in range(chunks):
        hidden, gate_grad, up_grad, p0, p1, p2a, p2b, p3 = call(
            expert_kernel,
            [((rows_here, ff), bf16)] * 3
            + [((rows_here, columns), bf16)] * 2
            + [((half, columns), bf16)] * 2
            + [((rows_here, columns), bf16)],
            [tp, *gathered[c], expert_gate, expert_up, expert_down],
            "expert_chunk",
            flops=10 * rows_here * width * ff,
        )
        saved += [*gathered[c], hidden, gate_grad, up_grad]
        nothing = jnp.zeros((half, columns), bf16)
        to_next = lax.ppermute(p2a, "tp", right)
        to_last = lax.ppermute(p2b, "tp", left)
        p1 = (p1.astype(f32) + jnp.concatenate([to_next, nothing]).astype(f32)).astype(bf16)
        p3 = (p3.astype(f32) + jnp.concatenate([nothing, to_last]).astype(f32)).astype(bf16)
        from_last = lax.ppermute(p1, "tp", right)
        from_next = lax.ppermute(p3, "tp", left)
        slot_grad = (p0.astype(f32) + from_last.astype(f32) + from_next.astype(f32)).astype(bf16)
        returned.append(exchange(slot_grad.reshape(sp_size, part, columns), "sp"))

    grad_gate, grad_up, grad_down = call(
        weights_kernel,
        [(expert_gate.shape, f32), (expert_up.shape, f32), (expert_down.shape, f32)],
        [tp, *saved],
        "expert_weights",
        flops=6 * sp_size * capacity * width * ff,
    )

    product = in_gate.astype(f32) * conv_input.astype(f32)
    earlier = shift_edge(product[-2:], "sp", 1)
    extended = jnp.concatenate([earlier, product], axis=0)
    filtered = conv_taps[0] * product + conv_taps[1] * extended[1:-1] + conv_taps[2] * extended[:-2]
    mixed_in = (out_gate.astype(f32) * filtered).astype(bf16)

    (token_cols,) = call(
        token_kernel,
        [((tokens, columns), bf16)],
        [tp, *(x for pair in zip(picks, returned) for x in pair)],
        "token_sum",
    )
    t3 = lax.ppermute(token_cols, "tp", right)
    t1 = lax.ppermute(token_cols, "tp", left)
    t2a = lax.ppermute(t3[: tokens // 2], "tp", right)
    t2b = lax.ppermute(t1[tokens // 2 :], "tp", left)
    grad_stream, grad_out_gate, filtered_grad, weight_grad = call(
        tail_kernel,
        [
            ((tokens, columns), bf16),
            (out_gate.shape, bf16),
            (out_gate.shape, f32),
            (out_weight.shape, bf16),
        ],
        [tp, token_cols, t1, t2a, t2b, t3, stream_in, cotangent, gain, out_weight, filtered, out_gate, mixed_in],
        "stream_tail",
    )
    later = shift_edge(filtered_grad[:2], "sp", -1)
    extended_grad = jnp.concatenate([filtered_grad, later], axis=0)
    product_grad = (
        conv_taps[0] * filtered_grad
        + conv_taps[1] * extended_grad[1:-1]
        + conv_taps[2] * extended_grad[2:]
    )
    grad_in_gate = (product_grad * conv_input.astype(f32)).astype(bf16)
    grad_conv_input = (product_grad * in_gate.astype(f32)).astype(bf16)

    core = lax.rem(lax.axis_index("sp"), 2)
    pairs = weight_grad.reshape(sp_size // 2, 2, width // sp_size, out_weight.shape[1])
    keep = lax.dynamic_index_in_dim(pairs, core, 1, keepdims=False)
    give = lax.dynamic_index_in_dim(pairs, 1 - core, 1, keepdims=False)
    taken = lax.ppermute(give, "sp", [(k, k ^ 1) for k in range(sp_size)])
    keep = (keep.astype(f32) + taken.astype(f32)).astype(bf16)
    same_core = [[2 * k + c for k in range(sp_size // 2)] for c in range(2)]
    grad_out_weight = exchange(keep, "sp", same_core).astype(f32).sum(axis=0)
    return (
        grad_stream, grad_out_gate, grad_in_gate, grad_conv_input, grad_out_weight,
        grad_gate, grad_up, grad_down,
    )


def solution(mesh):
    return jax.shard_map(
        shards,
        mesh=mesh,
        in_specs=(
            P("sp", None), P("sp", None), P(), P("sp", "tp"), P("sp", "tp"), P("sp", "tp"),
            P(None, "tp"), P(None, "tp"), P("sp", None, "tp"), P("sp", None, "tp"),
            P("sp", "tp", None), P("sp", None), P("sp", None),
        ),
        out_specs=(
            P("sp", "tp"), P("sp", "tp"), P("sp", "tp"), P("sp", "tp"), P("sp", "tp"),
            P("sp", None, "tp"), P("sp", None, "tp"), P("sp", "tp", None),
        ),
        check_vma=False,
    )
```

```python
import jax
import jax.numpy as jnp
from jax import lax
from jax.experimental import pallas as pl
from jax.experimental.pallas import tpu as pltpu
from jax.sharding import PartitionSpec as P


norm_eps = 1e-06
bf16 = jnp.bfloat16
f32 = jnp.float32


WHOLE = pl.BlockSpec(memory_space=pltpu.VMEM)
SCALAR = pl.BlockSpec(memory_space=pltpu.SMEM)


def call(body, outs, operands, flops=0, moved=0, limit=60 * 1024 * 1024, scalars=1):
    return pl.pallas_call(
        body,
        out_shape=[jax.ShapeDtypeStruct(shape, dtype) for shape, dtype in outs],
        in_specs=[SCALAR] * scalars + [WHOLE] * (len(operands) - scalars),
        out_specs=[WHOLE] * len(outs),
        cost_estimate=pl.CostEstimate(flops=flops, bytes_accessed=moved, transcendentals=0),
        compiler_params=pltpu.CompilerParams(vmem_limit_bytes=limit),
    )(*operands)


def dot(left, right, contract):
    return lax.dot_general(
        left, right, ((contract[:1], contract[1:]), ((), ())), preferred_element_type=f32
    )


def ring(size, steps):
    return [(k, (k + steps) % size) for k in range(size)]


def send_kernel(tp_ref, choice_ref, scale_ref, stream_ref, gain_ref, cot_ref, rms_ref, *outs):
    tokens, _ = stream_ref.shape
    chunks = len(outs) // 2
    experts, part, columns = outs[0].shape
    part = part // 2
    start = pl.multiple_of(tp_ref[0] * columns, columns)
    first_id, second_id = choice_ref[0:1, :], choice_ref[1:2, :]
    expert_iota = lax.broadcasted_iota(jnp.int32, (experts, tokens), 0)
    first, second = first_id == expert_iota, second_id == expert_iota
    named = jnp.where(first | second, 1.0, 0.0).astype(bf16)
    row = lax.broadcasted_iota(jnp.int32, (tokens, tokens), 0)
    col = lax.broadcasted_iota(jnp.int32, (tokens, tokens), 1)
    before = jnp.where(row < col, 1.0, 0.0).astype(bf16)
    earlier = dot(named, before, (1, 0))
    slots = []
    for chosen, ids in ((first, first_id), (second, second_id)):
        place = jnp.sum(jnp.where(chosen, earlier, 0.0), axis=0, keepdims=True).astype(jnp.int32)
        chunk = lax.div(place, part)
        slots.append(chunk * (experts * part) + ids * part + (place - chunk * part))
    stream = stream_ref[...].astype(f32)
    inverse_rms = lax.rsqrt(jnp.mean(stream * stream, axis=-1, keepdims=True) + norm_eps)
    rms_ref[...] = inverse_rms
    stream_cols = stream_ref[:, pl.ds(start, columns)].astype(f32)
    normed = (stream_cols * inverse_rms * gain_ref[:, pl.ds(start, columns)]).astype(bf16)
    cot = cot_ref[:, pl.ds(start, columns)]
    slot_iota = lax.broadcasted_iota(jnp.int32, (experts * part, tokens), 0)
    for c in range(chunks):
        send_ref, pick_ref = outs[2 * c : 2 * c + 2]
        here = slot_iota + c * experts * part
        pick_first, pick_second = slots[0] == here, slots[1] == here
        pick = jnp.where(pick_first | pick_second, 1.0, 0.0).astype(bf16)
        pick_ref[...] = pick
        send_ref[:, :part, :] = dot(pick, normed, (1, 0)).astype(bf16).reshape(experts, part, columns)
        scale = jnp.where(pick_first, scale_ref[0:1, :], 0.0) + jnp.where(
            pick_second, scale_ref[1:2, :], 0.0
        )
        weight = jnp.sum(scale, axis=1, keepdims=True)
        send_ref[:, part:, :] = (
            (dot(pick, cot, (1, 0)) * weight).astype(bf16).reshape(experts, part, columns)
        )


def block(ref, k, parts=2, half=None):
    part = ref.shape[1] // parts
    peers = slice(None)
    if half is not None:
        peers = pl.ds(pl.multiple_of(half * (ref.shape[0] // 2), ref.shape[0] // 2), ref.shape[0] // 2)
    return ref[peers, k * part : (k + 1) * part, :].reshape(-1, ref.shape[2])


def gathered_blocks(refs, half=None):
    own, after, before, far_rows, far_scaled = refs
    rows = [block(r, 0, p, half) for r, p in ((own, 2), (after, 2), (far_rows, 1), (before, 2))]
    scaled = [
        block(r, k, p, half)
        for r, k, p in ((own, 1, 2), (after, 1, 2), (far_scaled, 0, 1), (before, 1, 2))
    ]
    return rows, scaled


def column_starts(tp_ref, columns):
    return [pl.multiple_of(lax.rem(tp_ref[0] + j, 4) * columns, columns) for j in range(4)]


def for_each_half(rows, step):
    def one(half, carry):
        step(half, pl.ds(pl.multiple_of(half * (rows // 2), rows // 2), rows // 2))
        return carry

    lax.fori_loop(0, 2, one, 0)


def first_products(rows, scaled, gate_ref, up_ref, down_ref, starts):
    columns = rows[0].shape[1]
    gate_pre = up_pre = hidden_grad = 0.0
    for row, scaled_row, start in zip(rows, scaled, starts):
        gate_pre = gate_pre + dot(row, gate_ref[0, pl.ds(start, columns), :], (1, 0))
        up_pre = up_pre + dot(row, up_ref[0, pl.ds(start, columns), :], (1, 0))
        hidden_grad = hidden_grad + dot(scaled_row, down_ref[0, :, pl.ds(start, columns)], (1, 1))
    return gate_pre, up_pre, hidden_grad


def expert_start_kernel(tp_ref, own, after, before, gate_ref, up_ref, down_ref, *outs):
    starts = column_starts(tp_ref, own.shape[2])

    def step(half, here):
        sums = first_products(
            [block(ref, 0, 2, half) for ref in (own, after, before)],
            [block(ref, 1, 2, half) for ref in (own, after, before)],
            gate_ref, up_ref, down_ref, [starts[j] for j in (0, 1, 3)],
        )
        for ref, value in zip(outs, sums):
            ref[here, :] = value

    for_each_half(outs[0].shape[0], step)


def expert_kernel(tp_ref, *refs):
    weights, outs = refs[5:8], refs[8:]
    gate_ref, up_ref, _ = weights
    hidden_ref, ggrad_ref, ugrad_ref, *places = outs
    starts = column_starts(tp_ref, refs[0].shape[2])
    columns = refs[0].shape[2]

    def step(half, here):
        if len(refs[4].shape) == 3:
            rows, scaled = gathered_blocks(refs[:5], half)
            gate_pre, up_pre, hidden_grad = first_products(rows, scaled, *weights, starts)
        else:
            far = first_products(
                [block(refs[0], 0, 1, half)], [block(refs[1], 0, 1, half)], *weights, starts[2:3]
            )
            gate_pre, up_pre, hidden_grad = (
                ref[here, :] + value for ref, value in zip(refs[2:5], far)
            )
        sigmoid_gate = jax.nn.sigmoid(gate_pre)
        silu_gate = gate_pre * sigmoid_gate
        hidden_ref[here, :] = (silu_gate * up_pre).astype(bf16)
        gate_grad = (
            hidden_grad * up_pre * sigmoid_gate * (1.0 + gate_pre * (1.0 - sigmoid_gate))
        ).astype(bf16)
        up_grad = (hidden_grad * silu_gate).astype(bf16)
        ggrad_ref[here, :] = gate_grad
        ugrad_ref[here, :] = up_grad
        for place, start in zip(places, starts):
            place[here, :] = (
                dot(gate_grad, gate_ref[0, pl.ds(start, columns), :], (1, 1))
                + dot(up_grad, up_ref[0, pl.ds(start, columns), :], (1, 1))
            ).astype(bf16)

    for_each_half(hidden_ref.shape[0], step)


def weights_kernel(tp_ref, *refs):
    chunks = (len(refs) - 3) // 8
    outs = refs[-3:]
    columns = refs[0].shape[2]
    starts = column_starts(tp_ref, columns)
    part = refs[0].shape[1] // 2

    def step(half, here):
        for j in range(4):
            gate = up = down = 0.0
            for c in range(chunks):
                own, after, before, far_rows, far_scaled = refs[8 * c : 8 * c + 5]
                ref = (own, after, far_rows, before)[j]
                rows = ref[:, :part, here].reshape(-1, columns // 2)
                if j == 2:
                    scaled = far_scaled[:, :, here].reshape(-1, columns // 2)
                else:
                    scaled = ref[:, part:, here].reshape(-1, columns // 2)
                hidden, gate_grad, up_grad = (refs[8 * c + 5 + k][...] for k in range(3))
                gate = gate + dot(rows, gate_grad, (0, 0))
                up = up + dot(rows, up_grad, (0, 0))
                down = down + dot(hidden, scaled, (0, 0))
            cols = pl.ds(pl.multiple_of(starts[j] + half * (columns // 2), columns // 2), columns // 2)
            outs[0][0, cols, :] = gate
            outs[1][0, cols, :] = up
            outs[2][0, :, cols] = down

    for_each_half(columns, step)


def token_kernel(
    tp_ref, pick0, back0, pick1, back1, stream_ref, gain_ref, rms_ref, token_ref, sum_ref
):
    columns = token_ref.shape[1]
    start = column_starts(tp_ref, columns)[0]
    token = (
        dot(pick0[...], block(back0, 0, 1), (0, 0)) + dot(pick1[...], block(back1, 0, 1), (0, 0))
    ).astype(bf16)
    token_ref[...] = token
    unit = stream_ref[:, pl.ds(start, columns)].astype(f32) * rms_ref[...]
    unit_grad = token.astype(f32) * gain_ref[:, pl.ds(start, columns)]
    row_sum = jnp.sum(unit * unit_grad, axis=-1, keepdims=True)
    sum_ref[...] = jnp.transpose(jnp.broadcast_to(row_sum, (row_sum.shape[0], 128)))[0:1, :]


def stream_grads(token, cot, stream, gain, inverse_rms, along):
    unit = stream.astype(f32) * inverse_rms
    unit_grad = token.astype(f32) * gain
    return (cot.astype(f32) + inverse_rms * (unit_grad - unit * along)).astype(bf16)


def grad_kernel(
    tp_ref, core_ref, token_ref, s0, s1, s2, s3, stream_ref, cot_ref, gain_ref, rms_ref,
    m0, m1, m2, m3, gstream_ref, along_ref, keep_ref, give_ref,
):
    columns = token_ref.shape[1]
    start = column_starts(tp_ref, columns)[0]
    total = (s0[...] + s1[...] + s2[...] + s3[...]) * (1.0 / (4 * columns))
    along = jnp.transpose(jnp.broadcast_to(total, (128, total.shape[1])))[:, 0:1]
    along_ref[...] = along
    here = pl.ds(start, columns)
    grad = stream_grads(
        token_ref[...], cot_ref[:, here], stream_ref[:, here], gain_ref[:, here], rms_ref[...], along
    )
    gstream_ref[...] = grad
    products = [
        dot(grad, m[...], (0, 0)).astype(bf16).reshape(*keep_ref.shape[:1], *keep_ref.shape[2:])
        for m in (m0, m1, m2, m3)
    ]
    matching = lax.rem(tp_ref[0] + core_ref[0], 2) == 0
    places = [lax.rem(tp_ref[0] + j, 4) // 2 for j in range(4)]
    for j in (0, 2):
        even, odd = products[j][:, None], products[j + 1][:, None]
        even_at, odd_at = places[j], places[j + 1]
        keep_ref[:, pl.ds(jnp.where(matching, even_at, odd_at), 1)] = jnp.where(matching, even, odd)
        give_ref[:, pl.ds(jnp.where(matching, odd_at, even_at), 1)] = jnp.where(matching, odd, even)


def mixed_kernel(
    tp_ref, g0, t1, t2, t3, stream_ref, cot_ref, gain_ref, rms_ref, along_ref, weight_ref,
    filtered_ref, gate_ref, ggate_ref, fgrad_ref,
):
    columns = g0.shape[1]
    starts = column_starts(tp_ref, columns)
    mixed_grad = dot(g0[...], weight_ref[pl.ds(starts[0], columns), :], (1, 0))
    for token_ref, start in zip((t1, t2, t3), starts[1:]):
        here = pl.ds(start, columns)
        grad = stream_grads(
            token_ref[...], cot_ref[:, here], stream_ref[:, here], gain_ref[:, here], rms_ref[...],
            along_ref[...],
        )
        mixed_grad = mixed_grad + dot(grad, weight_ref[here, :], (1, 0))
    ggate_ref[...] = (mixed_grad * filtered_ref[...]).astype(bf16)
    fgrad_ref[...] = mixed_grad * gate_ref[...].astype(f32)


def shift_edge(value, axis, steps):
    count = lax.axis_size(axis)
    first, last = (max(0, -steps), min(count, count - steps))
    return lax.ppermute(value, axis, [(source, source + steps) for source in range(first, last)])


def exchange(array, axis, groups=None):
    return lax.all_to_all(
        array, axis, split_axis=0, concat_axis=0, tiled=True, axis_index_groups=groups
    )


def body(
    cotangent, stream_in, norm_gain, out_gate, in_gate, conv_input, conv_taps, out_weight,
    expert_gate, expert_up, expert_down, expert_choice, route_scale,
):
    sp_size = lax.axis_size("sp")
    tp_size = lax.axis_size("tp")
    tokens, width = stream_in.shape
    columns = width // tp_size
    capacity = 4 * tokens // sp_size
    chunks = 2
    part = capacity // chunks
    right, left = ring(tp_size, 1), ring(tp_size, -1)
    tp = lax.axis_index("tp").astype(jnp.int32).reshape(1)
    gain = norm_gain.reshape(1, width)

    sent_block = ((sp_size, 2 * part, columns), bf16)
    inverse_rms, *sent = call(
        send_kernel,
        [((tokens, 1), f32)] + [sent_block, ((sp_size * part, tokens), bf16)] * chunks,
        [tp, expert_choice.T, route_scale.T, stream_in, gain, cotangent],
    )
    picks = sent[1::2]

    def send_along(value, pairs):
        return lax.ppermute(value, "tp", pairs)

    gathered = []
    for c in range(chunks):
        own = exchange(sent[2 * c], "sp")
        before = send_along(own, right)
        after = send_along(own, left)
        far_rows = send_along(before[:, :part], right)
        far_scaled = send_along(after[:, part:], left)
        gathered.append([own, after, before, far_rows, far_scaled])

    returned = []
    saved = []
    rows_here = sp_size * part
    ff = expert_gate.shape[2]
    half = rows_here // 2
    for c in range(chunks):
        ahead = c < chunks - 1
        operands = gathered[c]
        weights = [expert_gate, expert_up, expert_down]
        if not ahead:
            started = call(
                expert_start_kernel,
                [((rows_here, ff), f32)] * 3,
                [tp, *operands[:3], *weights],
                flops=5 * rows_here * width * ff,
            )
            operands = [*operands[3:], *started]
        hidden, gate_grad, up_grad, p0, p1, p2, p3 = call(
            expert_kernel,
            [((rows_here, ff), bf16)] * 3 + [((rows_here, columns), bf16)] * 4,
            [tp, *operands, *weights],
            flops=10 * rows_here * width * ff,
        )
        saved += [*gathered[c], hidden, gate_grad, up_grad]
        if ahead:
            nothing = jnp.zeros((half, columns), bf16)
            to_next = send_along(p2[:half], right)
            to_last = send_along(p2[half:], left)
            p1 = (p1.astype(f32) + jnp.concatenate([to_next, nothing]).astype(f32)).astype(bf16)
            p3 = (p3.astype(f32) + jnp.concatenate([nothing, to_last]).astype(f32)).astype(bf16)
        from_last = send_along(p1, right)
        from_next = send_along(p3, left)
        slot_grad = p0.astype(f32) + from_last.astype(f32) + from_next.astype(f32)
        if not ahead:
            slot_grad = slot_grad + send_along(p2, ring(tp_size, 2)).astype(f32)
        slot_grad = slot_grad.astype(bf16).reshape(sp_size, part, columns)
        returned.append(exchange(slot_grad, "sp"))

    grad_gate, grad_up, grad_down = call(
        weights_kernel,
        [(expert_gate.shape, f32), (expert_up.shape, f32), (expert_down.shape, f32)],
        [tp, *saved],
        flops=6 * sp_size * capacity * width * ff,
    )

    product = in_gate.astype(f32) * conv_input.astype(f32)
    earlier = shift_edge(product[-2:], "sp", 1)
    extended = jnp.concatenate([earlier, product], axis=0)
    filtered = conv_taps[0] * product + conv_taps[1] * extended[1:-1] + conv_taps[2] * extended[:-2]
    mixed_in = (out_gate.astype(f32) * filtered).astype(bf16)

    from_peers = (left, ring(tp_size, 2), right)

    def to_peers(value):
        return [value] + [send_along(value, pairs) for pairs in from_peers]

    mixed_blocks = to_peers(mixed_in)
    token_cols, row_sum = call(
        token_kernel,
        [((tokens, columns), bf16), ((1, tokens), f32)],
        [tp, picks[0], returned[0], picks[1], returned[1], stream_in, gain, inverse_rms],
    )
    row_sums = to_peers(row_sum)
    token_blocks = to_peers(token_cols)
    core = lax.rem(lax.axis_index("sp"), 2).astype(jnp.int32).reshape(1)
    rows_out = width // sp_size
    pieces = ((columns // rows_out, tp_size // 2, rows_out, out_weight.shape[1]), bf16)
    grad_stream, along, keep, give = call(
        grad_kernel,
        [((tokens, columns), bf16), ((tokens, 1), f32), pieces, pieces],
        [
            tp, core, token_cols, *row_sums, stream_in, cotangent, gain, inverse_rms,
            *mixed_blocks,
        ],
        scalars=2,
    )
    grad_out_gate, filtered_grad = call(
        mixed_kernel,
        [(out_gate.shape, bf16), (out_gate.shape, f32)],
        [
            tp, grad_stream, *token_blocks[1:], stream_in, cotangent, gain, inverse_rms, along,
            out_weight, filtered, out_gate,
        ],
    )
    later = shift_edge(filtered_grad[:2], "sp", -1)
    extended_grad = jnp.concatenate([filtered_grad, later], axis=0)
    product_grad = (
        conv_taps[0] * filtered_grad
        + conv_taps[1] * extended_grad[1:-1]
        + conv_taps[2] * extended_grad[2:]
    )
    grad_in_gate = (product_grad * conv_input.astype(f32)).astype(bf16)
    grad_conv_input = (product_grad * in_gate.astype(f32)).astype(bf16)

    taken = lax.ppermute(give, "sp", [(k, k ^ 1) for k in range(sp_size)])
    keep = (keep.astype(f32) + taken.astype(f32)).astype(bf16)
    same_core = [[2 * k + c for k in range(sp_size // 2)] for c in range(2)]
    keep = keep.reshape(sp_size // 2, rows_out, out_weight.shape[1])
    reduced = exchange(keep, "sp", same_core).astype(f32).sum(axis=0)
    blocks = sp_size // tp_size
    placed = [
        (j * tp_size + q, (q * blocks + j // tp_size) * tp_size + j % tp_size)
        for j in range(sp_size)
        for q in range(tp_size)
    ]
    grad_out_weight = lax.ppermute(reduced, ("sp", "tp"), placed)
    return (
        grad_stream, grad_out_gate, grad_in_gate, grad_conv_input, grad_out_weight,
        grad_gate, grad_up, grad_down,
    )


def solution(mesh):
    return jax.shard_map(
        body,
        mesh=mesh,
        in_specs=(
            P("sp", None), P("sp", None), P(), P("sp", "tp"), P("sp", "tp"), P("sp", "tp"),
            P(None, "tp"), P(None, "tp"), P("sp", None, "tp"), P("sp", None, "tp"),
            P("sp", "tp", None), P("sp", None), P("sp", None),
        ),
        out_specs=(
            P("sp", "tp"), P("sp", "tp"), P("sp", "tp"), P("sp", "tp"), P("sp", "tp"),
            P("sp", None, "tp"), P("sp", None, "tp"), P("sp", "tp", None),
        ),
        check_vma=False,
    )
```

```python
import jax
import jax.numpy as jnp
from jax import lax
from jax.experimental import pallas as pl
from jax.experimental.pallas import tpu as pltpu
from jax.sharding import PartitionSpec as P


norm_eps = 1e-06
bf16 = jnp.bfloat16
f32 = jnp.float32


WHOLE = pl.BlockSpec(memory_space=pltpu.VMEM)
SCALAR = pl.BlockSpec(memory_space=pltpu.SMEM)


def call(body, outs, operands, flops=0, moved=0, limit=60 * 1024 * 1024, scalars=1):
    return pl.pallas_call(
        body,
        out_shape=[jax.ShapeDtypeStruct(shape, dtype) for shape, dtype in outs],
        in_specs=[SCALAR] * scalars + [WHOLE] * (len(operands) - scalars),
        out_specs=[WHOLE] * len(outs),
        cost_estimate=pl.CostEstimate(flops=flops, bytes_accessed=moved, transcendentals=0),
        compiler_params=pltpu.CompilerParams(vmem_limit_bytes=limit),
    )(*operands)


def dot(left, right, contract):
    return lax.dot_general(
        left, right, ((contract[:1], contract[1:]), ((), ())), preferred_element_type=f32
    )


def ring(size, steps):
    return [(k, (k + steps) % size) for k in range(size)]


def send_kernel(
    tp_ref, choice_ref, scale_ref, stream_ref, gain_ref, cot_ref, rms_ref, weight_ref, *outs
):
    tokens, _ = stream_ref.shape
    chunks = len(outs) // 2
    experts, part, columns = outs[0].shape
    part = part // 2
    start = pl.multiple_of(tp_ref[0] * columns, columns)
    first_id, second_id = choice_ref[0:1, :], choice_ref[1:2, :]
    expert_iota = lax.broadcasted_iota(jnp.int32, (experts, tokens), 0)
    first, second = first_id == expert_iota, second_id == expert_iota
    named = jnp.where(first | second, 1.0, 0.0).astype(bf16)
    row = lax.broadcasted_iota(jnp.int32, (tokens, tokens), 0)
    col = lax.broadcasted_iota(jnp.int32, (tokens, tokens), 1)
    before = jnp.where(row < col, 1.0, 0.0).astype(bf16)
    earlier = dot(named, before, (1, 0))
    slots = []
    for chosen, ids in ((first, first_id), (second, second_id)):
        place = jnp.sum(jnp.where(chosen, earlier, 0.0), axis=0, keepdims=True).astype(jnp.int32)
        chunk = lax.div(place, part)
        slots.append(chunk * (experts * part) + ids * part + (place - chunk * part))
    stream = stream_ref[...].astype(f32)
    inverse_rms = lax.rsqrt(jnp.mean(stream * stream, axis=-1, keepdims=True) + norm_eps)
    rms_ref[...] = inverse_rms
    stream_cols = stream_ref[:, pl.ds(start, columns)].astype(f32)
    normed = (stream_cols * inverse_rms * gain_ref[:, pl.ds(start, columns)]).astype(bf16)
    cot = cot_ref[:, pl.ds(start, columns)]
    slot_iota = lax.broadcasted_iota(jnp.int32, (experts * part, tokens), 0)
    for c in range(chunks):
        send_ref, pick_ref = outs[2 * c : 2 * c + 2]
        here = slot_iota + c * experts * part
        pick_first, pick_second = slots[0] == here, slots[1] == here
        pick = jnp.where(pick_first | pick_second, 1.0, 0.0).astype(bf16)
        pick_ref[...] = pick
        send_ref[:, :part, :] = dot(pick, normed, (1, 0)).astype(bf16).reshape(experts, part, columns)
        scale = jnp.where(pick_first, scale_ref[0:1, :], 0.0) + jnp.where(
            pick_second, scale_ref[1:2, :], 0.0
        )
        weight = jnp.sum(scale, axis=1, keepdims=True)
        if c == chunks - 1:
            weight_ref[...] = weight
        send_ref[:, part:, :] = (
            (dot(pick, cot, (1, 0)) * weight).astype(bf16).reshape(experts, part, columns)
        )


def send_far_kernel(
    tp_ref, pick_ref, weight_ref, rms_ref, stream_ref, gain_ref, cot_ref, send_ref
):
    experts, part, columns = send_ref.shape
    part = part // 2
    here = pl.ds(column_starts(tp_ref, columns)[2], columns)
    pick = pick_ref[...]
    normed = (stream_ref[:, here].astype(f32) * rms_ref[...] * gain_ref[:, here]).astype(bf16)
    send_ref[:, :part, :] = dot(pick, normed, (1, 0)).astype(bf16).reshape(experts, part, columns)
    send_ref[:, part:, :] = (
        (dot(pick, cot_ref[:, here], (1, 0)) * weight_ref[...])
        .astype(bf16)
        .reshape(experts, part, columns)
    )


def block(ref, k, parts=2, half=None):
    part = ref.shape[1] // parts
    peers = slice(None)
    if half is not None:
        peers = pl.ds(pl.multiple_of(half * (ref.shape[0] // 2), ref.shape[0] // 2), ref.shape[0] // 2)
    return ref[peers, k * part : (k + 1) * part, :].reshape(-1, ref.shape[2])


def gathered_blocks(refs, half=None):
    own, after, before, *far = refs
    far = [(far[0], 0, 2), (far[0], 1, 2)] if len(far) == 1 else [(far[0], 0, 1), (far[1], 0, 1)]
    rows = [block(r, k, p, half) for r, k, p in ((own, 0, 2), (after, 0, 2), far[0], (before, 0, 2))]
    scaled = [
        block(r, k, p, half) for r, k, p in ((own, 1, 2), (after, 1, 2), far[1], (before, 1, 2))
    ]
    return rows, scaled


def column_starts(tp_ref, columns):
    return [pl.multiple_of(lax.rem(tp_ref[0] + j, 4) * columns, columns) for j in range(4)]


def for_each_half(rows, step):
    def one(half, carry):
        step(half, pl.ds(pl.multiple_of(half * (rows // 2), rows // 2), rows // 2))
        return carry

    lax.fori_loop(0, 2, one, 0)


def first_products(rows, scaled, gate_ref, up_ref, down_ref, starts):
    columns = rows[0].shape[1]
    gate_pre = up_pre = hidden_grad = 0.0
    for row, scaled_row, start in zip(rows, scaled, starts):
        gate_pre = gate_pre + dot(row, gate_ref[0, pl.ds(start, columns), :], (1, 0))
        up_pre = up_pre + dot(row, up_ref[0, pl.ds(start, columns), :], (1, 0))
        hidden_grad = hidden_grad + dot(scaled_row, down_ref[0, :, pl.ds(start, columns)], (1, 1))
    return gate_pre, up_pre, hidden_grad


def expert_start_kernel(tp_ref, own, after, before, gate_ref, up_ref, down_ref, *outs):
    starts = column_starts(tp_ref, own.shape[2])

    def step(half, here):
        sums = first_products(
            [block(ref, 0, 2, half) for ref in (own, after, before)],
            [block(ref, 1, 2, half) for ref in (own, after, before)],
            gate_ref, up_ref, down_ref, [starts[j] for j in (0, 1, 3)],
        )
        for ref, value in zip(outs, sums):
            ref[here, :] = value

    for_each_half(outs[0].shape[0], step)


def expert_kernel(tp_ref, *refs):
    given = len(refs) - 10
    weights, outs = refs[given : given + 3], refs[given + 3 :]
    gate_ref, up_ref, _ = weights
    hidden_ref, ggrad_ref, ugrad_ref, *places = outs
    starts = column_starts(tp_ref, refs[0].shape[2])
    columns = refs[0].shape[2]

    def step(half, here):
        if given == 5:
            rows, scaled = gathered_blocks(refs[:5], half)
            gate_pre, up_pre, hidden_grad = first_products(rows, scaled, *weights, starts)
        else:
            far = first_products(
                [block(refs[0], 0, 2, half)], [block(refs[0], 1, 2, half)], *weights, starts[2:3]
            )
            gate_pre, up_pre, hidden_grad = (
                ref[here, :] + value for ref, value in zip(refs[1:4], far)
            )
        sigmoid_gate = jax.nn.sigmoid(gate_pre)
        silu_gate = gate_pre * sigmoid_gate
        hidden_ref[here, :] = (silu_gate * up_pre).astype(bf16)
        gate_grad = (
            hidden_grad * up_pre * sigmoid_gate * (1.0 + gate_pre * (1.0 - sigmoid_gate))
        ).astype(bf16)
        up_grad = (hidden_grad * silu_gate).astype(bf16)
        ggrad_ref[here, :] = gate_grad
        ugrad_ref[here, :] = up_grad
        for place, start in zip(places, starts):
            place[here, :] = (
                dot(gate_grad, gate_ref[0, pl.ds(start, columns), :], (1, 1))
                + dot(up_grad, up_ref[0, pl.ds(start, columns), :], (1, 1))
            ).astype(bf16)

    for_each_half(hidden_ref.shape[0], step)


def weights_kernel(tp_ref, *refs):
    outs = refs[-3:]
    groups = ((refs[:5], refs[5:8]), (refs[8:12], refs[12:15]))
    columns = refs[0].shape[2]
    starts = column_starts(tp_ref, columns)
    part = refs[0].shape[1] // 2

    def step(half, here):
        for j in range(4):
            gate = up = down = 0.0
            for (own, after, before, *far), results in groups:
                ref = (own, after, far[0], before)[j]
                rows = ref[:, :part, here].reshape(-1, columns // 2)
                if j == 2 and len(far) == 2:
                    scaled = far[1][:, :, here].reshape(-1, columns // 2)
                else:
                    scaled = ref[:, part:, here].reshape(-1, columns // 2)
                hidden, gate_grad, up_grad = (r[...] for r in results)
                gate = gate + dot(rows, gate_grad, (0, 0))
                up = up + dot(rows, up_grad, (0, 0))
                down = down + dot(hidden, scaled, (0, 0))
            cols = pl.ds(pl.multiple_of(starts[j] + half * (columns // 2), columns // 2), columns // 2)
            outs[0][0, cols, :] = gate
            outs[1][0, cols, :] = up
            outs[2][0, :, cols] = down

    for_each_half(columns, step)


def token_kernel(
    tp_ref, pick0, back0, pick1, back1, stream_ref, gain_ref, rms_ref, token_ref, sum_ref
):
    columns = token_ref.shape[1]
    start = column_starts(tp_ref, columns)[0]
    token = (
        dot(pick0[...], block(back0, 0, 1), (0, 0)) + dot(pick1[...], block(back1, 0, 1), (0, 0))
    ).astype(bf16)
    token_ref[...] = token
    unit = stream_ref[:, pl.ds(start, columns)].astype(f32) * rms_ref[...]
    unit_grad = token.astype(f32) * gain_ref[:, pl.ds(start, columns)]
    row_sum = jnp.sum(unit * unit_grad, axis=-1, keepdims=True)
    sum_ref[...] = jnp.transpose(jnp.broadcast_to(row_sum, (row_sum.shape[0], 128)))[0:1, :]


def stream_grads(token, cot, stream, gain, inverse_rms, along):
    unit = stream.astype(f32) * inverse_rms
    unit_grad = token.astype(f32) * gain
    return (cot.astype(f32) + inverse_rms * (unit_grad - unit * along)).astype(bf16)


def grad_kernel(
    tp_ref, core_ref, token_ref, s0, s1, s2, s3, stream_ref, cot_ref, gain_ref, rms_ref,
    m0, m1, m2, m3, gstream_ref, along_ref, keep_ref, give_ref,
):
    columns = token_ref.shape[1]
    start = column_starts(tp_ref, columns)[0]
    total = (s0[...] + s1[...] + s2[...] + s3[...]) * (1.0 / (4 * columns))
    along = jnp.transpose(jnp.broadcast_to(total, (128, total.shape[1])))[:, 0:1]
    along_ref[...] = along
    here = pl.ds(start, columns)
    grad = stream_grads(
        token_ref[...], cot_ref[:, here], stream_ref[:, here], gain_ref[:, here], rms_ref[...], along
    )
    gstream_ref[...] = grad
    products = [
        dot(grad, m[...], (0, 0)).astype(bf16).reshape(*keep_ref.shape[:1], *keep_ref.shape[2:])
        for m in (m0, m1, m2, m3)
    ]
    matching = lax.rem(tp_ref[0] + core_ref[0], 2) == 0
    places = [lax.rem(tp_ref[0] + j, 4) // 2 for j in range(4)]
    for j in (0, 2):
        even, odd = products[j][:, None], products[j + 1][:, None]
        even_at, odd_at = places[j], places[j + 1]
        keep_ref[:, pl.ds(jnp.where(matching, even_at, odd_at), 1)] = jnp.where(matching, even, odd)
        give_ref[:, pl.ds(jnp.where(matching, odd_at, even_at), 1)] = jnp.where(matching, odd, even)


def mixed_kernel(
    tp_ref, g0, t1, t2, t3, stream_ref, cot_ref, gain_ref, rms_ref, along_ref, weight_ref,
    filtered_ref, gate_ref, ggate_ref, fgrad_ref,
):
    columns = g0.shape[1]
    starts = column_starts(tp_ref, columns)
    mixed_grad = dot(g0[...], weight_ref[pl.ds(starts[0], columns), :], (1, 0))
    for token_ref, start in zip((t1, t2, t3), starts[1:]):
        here = pl.ds(start, columns)
        grad = stream_grads(
            token_ref[...], cot_ref[:, here], stream_ref[:, here], gain_ref[:, here], rms_ref[...],
            along_ref[...],
        )
        mixed_grad = mixed_grad + dot(grad, weight_ref[here, :], (1, 0))
    ggate_ref[...] = (mixed_grad * filtered_ref[...]).astype(bf16)
    fgrad_ref[...] = mixed_grad * gate_ref[...].astype(f32)


def shift_edge(value, axis, steps):
    count = lax.axis_size(axis)
    first, last = (max(0, -steps), min(count, count - steps))
    return lax.ppermute(value, axis, [(source, source + steps) for source in range(first, last)])


def exchange(array, axis, groups=None):
    return lax.all_to_all(
        array, axis, split_axis=0, concat_axis=0, tiled=True, axis_index_groups=groups
    )


def body(
    cotangent, stream_in, norm_gain, out_gate, in_gate, conv_input, conv_taps, out_weight,
    expert_gate, expert_up, expert_down, expert_choice, route_scale,
):
    sp_size = lax.axis_size("sp")
    tp_size = lax.axis_size("tp")
    tokens, width = stream_in.shape
    columns = width // tp_size
    capacity = 4 * tokens // sp_size
    chunks = 2
    part = capacity // chunks
    right, left = ring(tp_size, 1), ring(tp_size, -1)
    tp = lax.axis_index("tp").astype(jnp.int32).reshape(1)
    gain = norm_gain.reshape(1, width)

    sent_block = ((sp_size, 2 * part, columns), bf16)
    inverse_rms, far_weight, *sent = call(
        send_kernel,
        [((tokens, 1), f32), ((sp_size * part, 1), f32)]
        + [sent_block, ((sp_size * part, tokens), bf16)] * chunks,
        [tp, expert_choice.T, route_scale.T, stream_in, gain, cotangent],
    )
    picks = sent[1::2]

    def send_along(value, pairs):
        return lax.ppermute(value, "tp", pairs)

    (sent_far,) = call(
        send_far_kernel,
        [sent_block],
        [tp, picks[1], far_weight, inverse_rms, stream_in, gain, cotangent],
    )

    gathered = []
    for c in range(chunks):
        own = exchange(sent[2 * c], "sp")
        before = send_along(own, right)
        after = send_along(own, left)
        if c == 0:
            far_rows = send_along(before[:, :part], right)
            far_scaled = send_along(after[:, part:], left)
            far = [far_rows, far_scaled]
        else:
            far = [exchange(sent_far, "sp")]
        gathered.append([own, after, before, *far])

    returned = []
    saved = []
    rows_here = sp_size * part
    ff = expert_gate.shape[2]
    half = rows_here // 2
    for c in range(chunks):
        ahead = c < chunks - 1
        operands = gathered[c]
        weights = [expert_gate, expert_up, expert_down]
        if not ahead:
            started = call(
                expert_start_kernel,
                [((rows_here, ff), f32)] * 3,
                [tp, *operands[:3], *weights],
                flops=5 * rows_here * width * ff,
            )
            operands = [*operands[3:], *started]
        hidden, gate_grad, up_grad, p0, p1, p2, p3 = call(
            expert_kernel,
            [((rows_here, ff), bf16)] * 3 + [((rows_here, columns), bf16)] * 4,
            [tp, *operands, *weights],
            flops=10 * rows_here * width * ff,
        )
        saved += [*gathered[c], hidden, gate_grad, up_grad]
        if ahead:
            nothing = jnp.zeros((half, columns), bf16)
            to_next = send_along(p2[:half], right)
            to_last = send_along(p2[half:], left)
            p1 = (p1.astype(f32) + jnp.concatenate([to_next, nothing]).astype(f32)).astype(bf16)
            p3 = (p3.astype(f32) + jnp.concatenate([nothing, to_last]).astype(f32)).astype(bf16)
        from_last = send_along(p1, right)
        from_next = send_along(p3, left)
        slot_grad = p0.astype(f32) + from_last.astype(f32) + from_next.astype(f32)
        if not ahead:
            slot_grad = slot_grad + send_along(p2, ring(tp_size, 2)).astype(f32)
        slot_grad = slot_grad.astype(bf16).reshape(sp_size, part, columns)
        returned.append(exchange(slot_grad, "sp"))

    grad_gate, grad_up, grad_down = call(
        weights_kernel,
        [(expert_gate.shape, f32), (expert_up.shape, f32), (expert_down.shape, f32)],
        [tp, *saved],
        flops=6 * sp_size * capacity * width * ff,
    )

    product = in_gate.astype(f32) * conv_input.astype(f32)
    earlier = shift_edge(product[-2:], "sp", 1)
    extended = jnp.concatenate([earlier, product], axis=0)
    filtered = conv_taps[0] * product + conv_taps[1] * extended[1:-1] + conv_taps[2] * extended[:-2]
    mixed_in = (out_gate.astype(f32) * filtered).astype(bf16)

    from_peers = (left, ring(tp_size, 2), right)

    def to_peers(value):
        return [value] + [send_along(value, pairs) for pairs in from_peers]

    mixed_blocks = to_peers(mixed_in)
    token_cols, row_sum = call(
        token_kernel,
        [((tokens, columns), bf16), ((1, tokens), f32)],
        [tp, picks[0], returned[0], picks[1], returned[1], stream_in, gain, inverse_rms],
    )
    row_sums = to_peers(row_sum)
    token_blocks = to_peers(token_cols)
    core = lax.rem(lax.axis_index("sp"), 2).astype(jnp.int32).reshape(1)
    rows_out = width // sp_size
    pieces = ((columns // rows_out, tp_size // 2, rows_out, out_weight.shape[1]), bf16)
    grad_stream, along, keep, give = call(
        grad_kernel,
        [((tokens, columns), bf16), ((tokens, 1), f32), pieces, pieces],
        [
            tp, core, token_cols, *row_sums, stream_in, cotangent, gain, inverse_rms,
            *mixed_blocks,
        ],
        scalars=2,
    )
    grad_out_gate, filtered_grad = call(
        mixed_kernel,
        [(out_gate.shape, bf16), (out_gate.shape, f32)],
        [
            tp, grad_stream, *token_blocks[1:], stream_in, cotangent, gain, inverse_rms, along,
            out_weight, filtered, out_gate,
        ],
    )
    later = shift_edge(filtered_grad[:2], "sp", -1)
    extended_grad = jnp.concatenate([filtered_grad, later], axis=0)
    product_grad = (
        conv_taps[0] * filtered_grad
        + conv_taps[1] * extended_grad[1:-1]
        + conv_taps[2] * extended_grad[2:]
    )
    grad_in_gate = (product_grad * conv_input.astype(f32)).astype(bf16)
    grad_conv_input = (product_grad * in_gate.astype(f32)).astype(bf16)

    taken = lax.ppermute(give, "sp", [(k, k ^ 1) for k in range(sp_size)])
    keep = (keep.astype(f32) + taken.astype(f32)).astype(bf16)
    same_core = [[2 * k + c for k in range(sp_size // 2)] for c in range(2)]
    keep = keep.reshape(sp_size // 2, rows_out, out_weight.shape[1])
    reduced = exchange(keep, "sp", same_core).astype(f32).sum(axis=0)
    blocks = sp_size // tp_size
    placed = [
        (j * tp_size + q, (q * blocks + j // tp_size) * tp_size + j % tp_size)
        for j in range(sp_size)
        for q in range(tp_size)
    ]
    grad_out_weight = lax.ppermute(reduced, ("sp", "tp"), placed)
    return (
        grad_stream, grad_out_gate, grad_in_gate, grad_conv_input, grad_out_weight,
        grad_gate, grad_up, grad_down,
    )


def solution(mesh):
    return jax.shard_map(
        body,
        mesh=mesh,
        in_specs=(
            P("sp", None), P("sp", None), P(), P("sp", "tp"), P("sp", "tp"), P("sp", "tp"),
            P(None, "tp"), P(None, "tp"), P("sp", None, "tp"), P("sp", None, "tp"),
            P("sp", "tp", None), P("sp", None), P("sp", None),
        ),
        out_specs=(
            P("sp", "tp"), P("sp", "tp"), P("sp", "tp"), P("sp", "tp"), P("sp", "tp"),
            P("sp", None, "tp"), P("sp", None, "tp"), P("sp", "tp", None),
        ),
        check_vma=False,
    )
```
